512 devices in a mesh: grp: 2 (over y), fs: 32 (over z, core), tp: 8 (over x).
Axes of the slice: x: 8, y: 2, z: 16, core: 2. Of those that a mesh axis runs over, the one named last changes fastest.
The devices are a block of a 8x8x16 slice.
Arguments:
- tokens: bfloat16 [32768, 2048], P(('grp', 'fs', 'tp')), parts along dimension 0, may hold values from -30 to 30
- gate_master: float32 [2048, 2752], P('fs', 'tp'), may hold values from -0.125 to 0.125
- up_master: float32 [2048, 2752], P('fs', 'tp'), may hold values from -0.125 to 0.125
- down_master: float32 [2048, 2752], P('fs', 'tp'), may hold values from -0.4375 to 0.4375
- norm_gain: float32 [2048], replicated, may hold values from 0.1 to 1.9
- post_gain: float32 [2048], replicated, may hold values from 0.1 to 1.9
- post_bias: float32 [2048], replicated, may hold values from -3 to 3
Outputs:
- gate_ready: bfloat16 [4096, 2752], P('grp', 'tp'), parts along dimension 0
- up_ready: bfloat16 [4096, 2752], P('grp', 'tp'), parts along dimension 0
- down_ready: bfloat16 [4096, 2752], P('grp', 'tp'), parts along dimension 0
- result: bfloat16 [32768, 2048], P(('grp', 'fs', 'tp')), parts along dimension 0
The draws below stay inside these ranges and needn't reach their ends.
There are 2 independent parts, one for each index of `grp`. The reference program is written for one: setup_inputs(seed, part) draws one part's arguments, and reference() takes and returns one part's arrays. A program takes and returns all parts, laid end to end along the dimension named above; an argument that names none is the same for every part. Nothing has to cross between parts.
All inputs are finite; a program needn't handle non-finite values.
Results may differ from the reference program's by a relative error of at most 0.009.
Values may be sent and summed in bfloat16 or wider, within the bound.
A program may use at most 64 MiB of HBM per device.

```python
import math
import jax
import jax.numpy as jnp
from jax import lax

D = 2048
FF = 2752
TOKENS = 16384
N_TP = 8


def draw_tokens(key, part):
    key_base, key_rows, key_cols = jax.random.split(key, 3)
    row_scale = jnp.exp(jax.random.uniform(key_rows, (TOKENS, 1), jnp.float32, math.log(0.3), math.log(3.0)))
    col_scale = jnp.exp(jax.random.uniform(key_cols, (1, D), jnp.float32, math.log(0.5), math.log(2.0)))
    base = jnp.clip(jax.random.normal(key_base, (TOKENS, D), jnp.float32), -4.0, 4.0)
    return (base * row_scale * col_scale).astype(jnp.bfloat16)


def shard_levels(rng, dims, pieces, least, top_value):
    gain = 1.0
    for axis_at, parts in pieces:
        draws = jax.random.uniform(jax.random.fold_in(jax.random.fold_in(rng, 6), axis_at), (parts,), jnp.float32, least / len(pieces), top_value / len(pieces))
        gain = gain * jnp.repeat(jnp.exp(draws), dims[axis_at] // parts).reshape((-1,) + (1,) * (len(dims) - 1 - axis_at))
    return gain


def centred(key, shape, deviation, most, cuts=(), kind=jnp.bfloat16):
    values = deviation * jax.random.normal(key, shape, jnp.float32)
    if cuts:
        values = values * shard_levels(key, shape, cuts, -0.22, 0.18)
    return jnp.clip(values, -most, most).astype(kind)


def setup_inputs(seed: int = 0, part: int = 0) -> dict:
    streams_of = jax.random.split(jax.random.key(seed), 8)
    part_keys = jax.random.split(jax.random.fold_in(streams_of[7], part), 8)
    return {
        "tokens": draw_tokens(jax.random.fold_in(jax.random.fold_in(streams_of[7], part), 71), part),
        "gate_master": centred(streams_of[1], (D, FF), D ** -0.5, 0.125, ((0, 32), (1, 8)), jnp.float32),
        "up_master": centred(streams_of[2], (D, FF), D ** -0.5, 0.125, ((0, 32), (1, 8)), jnp.float32),
        "down_master": centred(streams_of[3], (D, FF), (FF // 16) ** -0.5, 0.4375, ((0, 32), (1, 8)), jnp.float32),
        "norm_gain": jnp.clip(1.0 + 0.18 * jax.random.normal(streams_of[4], (D,), jnp.float32), 0.1, 1.9),
        "post_gain": jnp.clip(1.0 + 0.18 * jax.random.normal(streams_of[5], (D,), jnp.float32), 0.1, 1.9),
        "post_bias": centred(streams_of[6], (D,), 0.5, 3.0, (), jnp.float32),
    }


def reference(tokens, gate_master, up_master, down_master, norm_gain, post_gain, post_bias):
    gate_ready = (norm_gain[:, None] * gate_master).astype(jnp.bfloat16)
    up_ready = (norm_gain[:, None] * up_master).astype(jnp.bfloat16)
    down_ready = down_master.astype(jnp.bfloat16)
    wide = tokens.astype(jnp.float32)
    normed = (wide * lax.rsqrt(lax.optimization_barrier(jnp.mean(wide * wide, axis=-1, keepdims=True)) + 1e-06)).astype(jnp.bfloat16)
    gate = jnp.dot(normed, gate_ready, preferred_element_type=jnp.float32)
    upward = jnp.dot(normed, up_ready, preferred_element_type=jnp.float32)
    hidden = (jax.nn.silu(gate) * upward).astype(jnp.bfloat16)
    block_units = FF // N_TP
    branch = jnp.zeros((tokens.shape[0], D), jnp.float32)
    for block in range(N_TP):
        part_hidden = hidden[:, block * block_units:(block + 1) * block_units]
        part_down = down_ready[:, block * block_units:(block + 1) * block_units]
        partial_value = lax.dot_general(part_hidden, part_down, (((1,), (1,)), ((), ())), preferred_element_type=jnp.float32)
        rounded = lax.optimization_barrier(partial_value.astype(jnp.bfloat16))
        branch = branch + rounded.astype(jnp.float32)
    mixed = jnp.sqrt(jnp.float32(2.0)) * wide + 0.5 * branch
    center = lax.optimization_barrier(jnp.mean(mixed, axis=-1, keepdims=True))
    spread = lax.optimization_barrier(jnp.mean(jnp.square(mixed - center), axis=-1, keepdims=True))
    result = ((mixed - center) * lax.rsqrt(spread + 1e-05) * post_gain + post_bias).astype(jnp.bfloat16)
    return (gate_ready, up_ready, down_ready, result)
```

```python
import functools

import jax
import jax.numpy as jnp
from jax import lax
from jax.experimental import pallas as pl
from jax.experimental.pallas import tpu as pltpu
from jax.sharding import PartitionSpec as P

MESH = pl.DeviceIdType.MESH
CUTS = 4
VMEM_SPACE = pl.BlockSpec(memory_space=pltpu.VMEM)
ANY_SPACE = pl.BlockSpec(memory_space=pl.ANY)


def rows_of(index, size):
    return pl.ds(pl.multiple_of(index * size, size), size)


def gather_and_reduce(
    n_fs, n_tp, tokens, gate, up, down, gain, ready, branch,
    tok_in, w_in, normed, hidden, partial, sent, landed,
    in_sem, z_recv, z_send, core_recv, core_send, x_recv, x_send, r_recv, r_send,
):
    f, t = lax.axis_index("fs"), lax.axis_index("tp")
    block, width = tok_in.shape
    piece = w_in.shape[1]
    far_z, far_x = n_fs // 4, n_tp // 2
    side = width // 2
    cut = side // CUTS

    loads = [pltpu.make_async_copy(tokens, tok_in, in_sem.at[0])]
    for m, master in enumerate((gate, up, down)):
        loads.append(pltpu.make_async_copy(master, w_in.at[m], in_sem.at[1 + m]))
    for load in loads:
        load.start()

    z_next = (lax.rem(f + 2, n_fs), lax.rem(f + n_fs - 2, n_fs))
    x_next = (lax.rem(t + 1, n_tp), lax.rem(t + n_tp - 1, n_tp))
    other = f + 1 - 2 * lax.rem(f, 2)
    barrier = pltpu.get_barrier_semaphore()
    for there in ({"fs": z_next[0]}, {"fs": z_next[1]}, {"fs": other}, {"tp": x_next[0]}, {"tp": x_next[1]}):
        pl.semaphore_signal(barrier, inc=1, device_id=there, device_id_type=MESH)

    gain_row = gain[pl.ds(f // 2, 1), :]
    lane = lax.broadcasted_iota(jnp.int32, (piece, gain_row.shape[1]), 1)
    row = lax.broadcasted_iota(jnp.int32, (piece, gain_row.shape[1]), 0)
    gain_col = jnp.sum(
        jnp.where(lane == row + lax.rem(f, 2) * piece, gain_row, 0.0), axis=1, keepdims=True
    )
    own = rows_of(f, piece)
    for m in range(3):
        loads[1 + m].wait()
        value = w_in[m]
        if m < 2:
            value = gain_col * value
        ready[m, own, :] = value.astype(jnp.bfloat16)
    loads[0].wait()
    wide = tok_in[...].astype(jnp.float32)
    own_slot = (n_tp - 1) * block
    normed[pl.ds(own_slot, block), :] = (
        wide * lax.rsqrt(jnp.mean(wide * wide, axis=-1, keepdims=True) + 1e-06)
    ).astype(jnp.bfloat16)
    pl.semaphore_wait(barrier, 5)

    def z_rows(d, k):
        away = 2 * k if d == 0 else n_fs - 2 * k
        start = lax.rem(f + n_fs - away, n_fs) * piece
        if k < far_z:
            return pl.ds(pl.multiple_of(start, piece), piece)
        start = start + d * (piece // 2)
        return pl.ds(pl.multiple_of(start, piece // 2), piece // 2)

    def z_copy(d, k, m):
        rows = z_rows(d, k - 1) if k < far_z else None
        if rows is None:
            away = 2 * (k - 1) if d == 0 else n_fs - 2 * (k - 1)
            start = lax.rem(f + n_fs - away, n_fs) * piece + d * (piece // 2)
            rows = pl.ds(pl.multiple_of(start, piece // 2), piece // 2)
        ref = ready.at[m, rows, :]
        return pltpu.make_async_remote_copy(
            src_ref=ref, dst_ref=ref, send_sem=z_send.at[d, m], recv_sem=z_recv.at[d, k - 1, m],
            device_id={"fs": z_next[d]}, device_id_type=MESH,
        )

    def core_copy(rows, m):
        ref = ready.at[m, rows, :]
        return pltpu.make_async_remote_copy(
            src_ref=ref, dst_ref=ref, send_sem=core_send.at[m], recv_sem=core_recv.at[m],
            device_id={"fs": other}, device_id_type=MESH,
        )

    half = block // 2

    def slot(d, k):
        if k == 0:
            return own_slot
        return (2 * (k - 1) + (d if k < far_x else 0)) * block

    def x_copy(d, k, h):
        src = normed.at[pl.ds(slot(d, k - 1) + h * half, half), :]
        dst = normed.at[pl.ds(slot(d, k) + h * half, half), :]
        return pltpu.make_async_remote_copy(
            src_ref=src, dst_ref=dst, send_sem=x_send.at[d], recv_sem=x_recv.at[d, k - 1, h],
            device_id={"tp": x_next[d]}, device_id_type=MESH,
        )

    for d in range(2):
        for m in range(3):
            z_copy(d, 1, m).start()
        for h in range(2):
            x_copy(d, 1, h).start()
    for m in range(3):
        core_copy(own, m).start()

    events = []
    for k in range(1, far_z + 1):
        for m in range(3):
            size = 1.0 if k < far_z else 0.5
            events.append((1.9 + 3.15 * (k - 1) + 1.05 * size * (m + 1), "z", k, m))
    for k in range(1, far_x + 1):
        for h in range(2):
            events.append((1.9 + 5.6 * (k - 1) + 2.8 * (h + 1), "x", k, h))
    for _, kind, k, i in sorted(events):
        for d in range(2):
            if kind == "z":
                z_copy(d, k, i).wait_recv()
                if k < far_z:
                    z_copy(d, k + 1, i).start()
                core_copy(z_rows(d, k), i).start()
            else:
                if k == far_x and i != d:
                    continue
                x_copy(d, k, i).wait_recv()
                if k + 1 < far_x or (k + 1 == far_x and i == d):
                    x_copy(d, k + 1, i).start()
    for m in range(3):
        pltpu.make_async_copy(
            ready.at[m, pl.ds(0, n_fs // 2 * piece), :],
            ready.at[m, pl.ds(0, n_fs // 2 * piece), :],
            core_recv.at[m],
        ).wait()

    def compute(pair):
        rows = pl.ds(pair * 2 * block, 2 * block)
        x = normed[rows, :]
        g = jnp.dot(x, ready[0], preferred_element_type=jnp.float32)
        u = jnp.dot(x, ready[1], preferred_element_type=jnp.float32)
        hidden[rows, :] = (g * (1.0 / (1.0 + jnp.exp(-g))) * u).astype(jnp.bfloat16)
        h = hidden[rows, :]
        for j in range(width // cut):
            partial[j, rows, :] = lax.dot_general(
                h, ready[2, pl.ds(j * cut, cut), :], (((1,), (1,)), ((), ())),
                preferred_element_type=jnp.float32,
            ).astype(jnp.bfloat16)

    def r_copy(d, s, j):
        return pltpu.make_async_remote_copy(
            src_ref=sent.at[d, s, j], dst_ref=landed.at[d, s, j],
            send_sem=r_send.at[d], recv_sem=r_recv.at[d, s, j],
            device_id={"tp": x_next[d]}, device_id_type=MESH,
        )

    def r_slot(d, s):
        k = s + 1
        if k == n_tp:
            return own_slot
        return slot(d, k) if k <= far_x else slot(1 - d, n_tp - k)

    pairs = n_tp // 2
    for s in range(n_tp):
        if s < pairs:
            compute(s)
        for j in range(CUTS):
            for d in range(2):
                mine = partial[d * CUTS + j, pl.ds(r_slot(d, s), block), :].astype(jnp.float32)
                if s > 0:
                    r_copy(d, s - 1, j).wait_recv()
                    mine = mine + landed[d, s - 1, j].astype(jnp.float32)
                if s < n_tp - 1:
                    sent[d, s, j] = mine.astype(jnp.bfloat16)
                    r_copy(d, s, j).start()
                else:
                    branch[:, pl.ds(d * side + j * cut, cut)] = mine

    gone = pl.ds(0, (2 * far_z - 1) * piece // 2)
    for m in range(3):
        for d in range(2):
            pltpu.make_async_copy(ready.at[m, gone, :], ready.at[m, gone, :], z_send.at[d, m]).wait()
        pltpu.make_async_copy(
            ready.at[m, pl.ds(0, n_fs // 2 * piece), :],
            ready.at[m, pl.ds(0, n_fs // 2 * piece), :],
            core_send.at[m],
        ).wait()
    gone = pl.ds(0, (2 * far_x - 1) * half)
    for d in range(2):
        pltpu.make_async_copy(normed.at[gone, :], normed.at[gone, :], x_send.at[d]).wait()
        pltpu.make_async_copy(sent.at[d], sent.at[d], r_send.at[d]).wait()


def finish(ready, branch, tokens, post_gain, post_bias, gate, up, down, result, sem):
    for m, out in enumerate((gate, up, down)):
        pltpu.make_async_copy(ready.at[m], out, sem.at[m]).start()
    mixed = jnp.sqrt(jnp.float32(2.0)) * tokens[...].astype(jnp.float32) + 0.5 * branch[...]
    center = jnp.mean(mixed, axis=-1, keepdims=True)
    off = mixed - center
    spread = jnp.mean(jnp.square(off), axis=-1, keepdims=True)
    result[...] = (off * lax.rsqrt(spread + 1e-05) * post_gain[...] + post_bias[...]).astype(jnp.bfloat16)
    for m, out in enumerate((gate, up, down)):
        pltpu.make_async_copy(ready.at[m], out, sem.at[m]).wait()


def local(n_fs, n_tp, tokens, gate, up, down, norm_gain, post_gain, post_bias):
    block, width = tokens.shape
    piece, units = gate.shape
    far_z, far_x = n_fs // 4, n_tp // 2
    whole = n_fs * piece
    cut = width // 2 // CUTS
    steps = n_tp - 1
    bf16, f32 = jnp.bfloat16, jnp.float32
    dma = pltpu.SemaphoreType.DMA
    ready, branch = pl.pallas_call(
        functools.partial(gather_and_reduce, n_fs, n_tp),
        out_shape=(
            pltpu.VMEM((3, whole, units), bf16),
            pltpu.VMEM((block, width), f32),
        ),
        in_specs=[ANY_SPACE] * 4 + [VMEM_SPACE],
        out_specs=(VMEM_SPACE, VMEM_SPACE),
        scratch_shapes=[
            pltpu.VMEM((block, width), bf16),
            pltpu.VMEM((3, piece, units), f32),
            pltpu.VMEM((n_tp * block, width), bf16),
            pltpu.VMEM((n_tp * block, units), bf16),
            pltpu.VMEM((2 * CUTS, n_tp * block, cut), bf16),
            pltpu.VMEM((2, steps, CUTS, block, cut), bf16),
            pltpu.VMEM((2, steps, CUTS, block, cut), bf16),
            dma((4,)),
            dma((2, far_z, 3)),
            dma((2, 3)),
            dma((3,)),
            dma((3,)),
            dma((2, far_x, 2)),
            dma((2,)),
            dma((2, steps, CUTS)),
            dma((2,)),
        ],
        compiler_params=pltpu.CompilerParams(
            collective_id=0, has_side_effects=True, vmem_limit_bytes=40 * 1024 * 1024
        ),
    )(tokens, gate, up, down, norm_gain.reshape(-1, 2 * piece))
    return pl.pallas_call(
        finish,
        out_shape=(
            jax.ShapeDtypeStruct((whole, units), bf16),
            jax.ShapeDtypeStruct((whole, units), bf16),
            jax.ShapeDtypeStruct((whole, units), bf16),
            jax.ShapeDtypeStruct((block, width), bf16),
        ),
        in_specs=[VMEM_SPACE] * 5,
        out_specs=(ANY_SPACE, ANY_SPACE, ANY_SPACE, VMEM_SPACE),
        scratch_shapes=[dma((3,))],
        compiler_params=pltpu.CompilerParams(vmem_limit_bytes=24 * 1024 * 1024),
    )(ready, branch, tokens, post_gain.reshape(1, -1), post_bias.reshape(1, -1))


def solution(mesh):
    return jax.shard_map(
        functools.partial(local, mesh.shape["fs"], mesh.shape["tp"]),
        mesh=mesh,
        in_specs=(
            P(("grp", "fs", "tp"), None),
            P("fs", "tp"),
            P("fs", "tp"),
            P("fs", "tp"),
            P(),
            P(),
            P(),
        ),
        out_specs=(P("grp", "tp"), P("grp", "tp"), P("grp", "tp"), P(("grp", "fs", "tp"), None)),
        check_vma=False,
    )
```

```python
import functools

import jax
import jax.numpy as jnp
from jax import lax
from jax.experimental import pallas as pl
from jax.experimental.pallas import tpu as pltpu
from jax.sharding import PartitionSpec as P

MESH = pl.DeviceIdType.MESH
CUTS = 8
TOP = 8
PARTS = 3
VMEM_SPACE = pl.BlockSpec(memory_space=pltpu.VMEM)
HBM_SPACE = pl.BlockSpec(memory_space=pltpu.HBM)


def gather_and_reduce(
    n_fs, n_tp, units, tokens, gate, up, down, gain, post_gain, post_bias, ready, mixed, affine,
    tok_in, w_in, gain_in, normed, partial, sent, landed,
    in_sem, swap_sem, a_recv, a_send, b_recv, b_send, c_recv, c_send, core_recv, core_send,
    x_recv, x_send, r_recv, r_send, first_in,
):
    f, t = lax.axis_index("fs"), lax.axis_index("tp")
    nz = n_fs // 2
    z, c = f // 2, lax.rem(f, 2)
    low = nz - TOP
    block, width = tok_in.shape
    piece = w_in.shape[1] // 2
    pair_cols = 2 * piece
    share = ready.shape[2] // 2
    far = n_tp // 2
    cut = width // CUTS
    other = f + 1 - 2 * c

    def remote(src, dst, send, recv, **there):
        return pltpu.make_async_remote_copy(
            src_ref=src, dst_ref=dst, send_sem=send, recv_sem=recv,
            device_id=there, device_id_type=MESH,
        )

    def near(step):
        return lax.rem(t + step + n_tp, n_tp)

    barrier = pltpu.get_barrier_semaphore()

    def greet(**there):
        pl.semaphore_signal(barrier, inc=1, device_id=there, device_id_type=MESH)

    greet(fs=other)
    for step in (1, -1, 2, -2):
        greet(tp=near(step))

    @pl.when(z > 0)
    def _():
        greet(fs=f - 2)

    @pl.when((z > 0) & (z < nz - 1))
    def _():
        greet(fs=f + 2)

    @pl.when(z == 0)
    def _():
        for i in range(TOP):
            greet(fs=c + 2 * (low + i))

    my_rows = pl.ds(pl.multiple_of(c * piece, piece), piece)
    masters = (gate, up, down)
    loads = [pltpu.make_async_copy(tokens, tok_in, in_sem.at[0])]
    loads.append(pltpu.make_async_copy(gain.at[pl.ds(z, 1), :], gain_in, in_sem.at[1]))
    for m in range(3):
        loads.append(pltpu.make_async_copy(masters[m], w_in.at[m, my_rows, :], in_sem.at[2 + m]))
    loads.append(pltpu.make_async_copy(post_gain, affine.at[0], in_sem.at[5]))
    loads.append(pltpu.make_async_copy(post_bias, affine.at[1], in_sem.at[6]))
    for load in loads:
        load.start()

    count = 5 + jnp.where(z > 1, 1, 0) + jnp.where(z < nz - 1, 1, 0) + jnp.where(z >= low, 1, 0)
    pl.semaphore_wait(barrier, count)

    @pl.when(z == 0)
    def _():
        pl.semaphore_signal(first_in, inc=1, device_id={"fs": f + 2}, device_id_type=MESH)

    swaps = []
    for m in range(3):
        swaps.append(remote(masters[m], w_in.at[m, my_rows, :], swap_sem.at[0, m], swap_sem.at[1, m], fs=other))
        swaps[m].start()

    own_slot = (n_tp - 1) * block

    def slot(d, k):
        if k == 0:
            return own_slot
        return (2 * (k - 1) + (d if k < far else 0)) * block

    half = block // 2

    def x_copy(d, k_from, k_to):
        size = half if k_to == far else block
        shift = d * half if k_to == far else 0
        step = k_to - k_from
        return remote(
            normed.at[pl.ds(slot(d, k_from) + shift, size), :],
            normed.at[pl.ds(slot(d, k_to) + shift, size), :],
            x_send.at[d], x_recv.at[d, k_to - 1], tp=near(step if d == 0 else -step),
        )

    loads[1].wait()
    lane = lax.broadcasted_iota(jnp.int32, (pair_cols, pair_cols), 1)
    row = lax.broadcasted_iota(jnp.int32, (pair_cols, pair_cols), 0)
    gain_col = jnp.sum(jnp.where(lane == row, gain_in[...], 0.0), axis=1, keepdims=True)

    for m in range(3):
        loads[2 + m].wait()
        swaps[m].wait()
        value = w_in[m]
        if m < 2:
            value = gain_col * value
        ready[z, m, pl.ds(0, units), :] = value.T.astype(jnp.bfloat16)
        ready[z, m, pl.ds(units, 2 * share - units), :] = jnp.zeros(
            (2 * share - units, pair_cols), jnp.bfloat16
        )

    def part(i, index):
        if i < 2:
            return ready.at[index, c, pl.ds(i * share, share), :]
        return ready.at[index, 2, pl.ds(pl.multiple_of(c * share, 16), share), :]

    def a_copy(i, j, index):
        ref = part(i, index)
        return remote(ref, ref, a_send.at[j - 1], a_recv.at[j - 1, i], fs=f + 2)

    def b_copy(i, j, index):
        ref = part(i, index)
        return remote(ref, ref, b_send.at[j - 1], b_recv.at[j - 1, i], fs=f - 2)

    def c_copy(i, j, index, there):
        ref = part(i, index)
        return remote(ref, ref, c_send.at[j], c_recv.at[j, i], fs=there)

    def core_copy(i, index):
        ref = part(i, index)
        return remote(ref, ref, core_send.at[i], core_recv.at[i], fs=other)

    goes_right = z < nz - 1
    goes_left = (z > 1) & (z != low)
    passes_top = z < low - 1

    @pl.when(z >= low)
    def _():
        for i in range(PARTS):
            c_copy(i, z - low, z, c).start()

    @pl.when(goes_left)
    def _():
        for i in range(PARTS):
            b_copy(i, 1, z).start()

    @pl.when(goes_right)
    def _():
        for i in range(PARTS):
            a_copy(i, 1, z).start()

    loads[0].wait()
    wide = tok_in[...].astype(jnp.float32)
    normed[pl.ds(own_slot, block), :] = (
        wide * lax.rsqrt(jnp.mean(wide * wide, axis=-1, keepdims=True) + 1e-06)
    ).astype(jnp.bfloat16)
    for k in (2, 1):
        for d in range(2):
            x_copy(d, 0, k).start()

    left_most = max(low, TOP) - 1
    last_left = jnp.where(z < low, low - 1, nz - 1)
    events = []
    for j in range(1, nz - 1):
        events.append((2.0 + 2.83 * j, "a", j))
    for j in range(1, left_most + 1):
        events.append((3.0 + 5.2 * j, "b", j))
    for j in range(TOP):
        events.append((2.0 * low + 18.0 + 2.83 * j, "c", j))
    events.append((16.0, "x", 0))
    events.append((2.0 * low + 17.0, "first", 0))
    events.append((3.1 + 5.2 * (low - 2), "zero", 0))
    for j in range(1, low):
        events.append((1000.0 + j, "end", j))
    for _, kind, j in sorted(events):
        if kind == "x":
            for d in range(2):
                x_copy(d, 0, 2).wait_recv()
                for k in (far, 3):
                    x_copy(d, 2, k).start()
        if kind == "zero":

            @pl.when(z == 1)
            def _():
                pl.semaphore_wait(first_in, 1)
                for q in range(1, low):
                    for i in range(PARTS):
                        b_copy(i, q, q).start()

        if kind == "end":

            @pl.when(z == 0)
            def _():
                for i in range(PARTS):
                    b_copy(i, j, j).wait_recv()
                    core_copy(i, j).start()

        if kind == "first":

            @pl.when(z > 0)
            def _():
                for i in range(PARTS):
                    a_copy(i, z, 0).wait_recv()

                    @pl.when(goes_right)
                    def _():
                        a_copy(i, z + 1, 0).start()

                    core_copy(i, 0).start()

        if kind == "a":

            @pl.when(z > j)
            def _():
                for i in range(PARTS):
                    a_copy(i, j, z - j).wait_recv()

                    @pl.when(goes_right)
                    def _():
                        a_copy(i, j + 1, z - j).start()

                    core_copy(i, z - j).start()

        if kind == "b":

            @pl.when((z > 0) & (z + j <= last_left))
            def _():
                for i in range(PARTS):
                    b_copy(i, j, z + j).wait_recv()

                    @pl.when(goes_left)
                    def _():
                        b_copy(i, j + 1, z + j).start()

                    core_copy(i, z + j).start()

        if kind == "c":

            @pl.when(z < low)
            def _():
                for i in range(PARTS):
                    c_copy(i, j, low + j, c).wait_recv()

                    @pl.when(passes_top)
                    def _():
                        c_copy(i, j, low + j, f + 2).start()

                    core_copy(i, low + j).start()

    all_others = pl.ds(0, nz - 1)
    for i in range(PARTS):
        ref = ready.at[all_others, 0, pl.ds(0, share), :]
        pltpu.make_async_copy(ref, ref, core_recv.at[i]).wait()

    def cut_of(m, j):
        each = cut // pair_cols
        return jnp.concatenate([ready[j * each + i, m, pl.ds(0, units), :] for i in range(each)], axis=1)

    def compute(k):
        for d in range(2):
            if k == far:
                x_copy(d, 2, far).wait_recv()
            elif k != 2:
                x_copy(d, 0 if k == 1 else 2, k).wait_recv()
        rows = pl.ds(slot(0, k), 2 * block)
        dims = (((1,), (1,)), ((), ()))
        g = u = None
        for j in range(CUTS):
            x = normed[rows, pl.ds(j * cut, cut)]
            g_more = lax.dot_general(x, cut_of(0, j), dims, preferred_element_type=jnp.float32)
            u_more = lax.dot_general(x, cut_of(1, j), dims, preferred_element_type=jnp.float32)
            g = g_more if j == 0 else g + g_more
            u = u_more if j == 0 else u + u_more
        h = (g * (1.0 / (1.0 + jnp.exp(-g))) * u).astype(jnp.bfloat16)
        for j in range(CUTS):
            partial[j, rows, :] = jnp.dot(
                h, cut_of(2, j), preferred_element_type=jnp.float32
            ).astype(jnp.bfloat16)

    def r_copy(d, s, j):
        return remote(
            sent.at[d, s, j], landed.at[d, s, j], r_send.at[d, min(s, 1)], r_recv.at[d, s, j],
            tp=near(1 - 2 * d),
        )

    side = CUTS // 2
    for s in range(far):
        k = far - s
        compute(k)
        for at in range(side if s == 0 else CUTS):
            for d in range(2):
                j = d * side + at if s == 0 else ((1 - d) * side + at) % CUTS
                value = partial[j, pl.ds(slot(1 - d, k), block), :]
                if s > 0 and not (s == 1 and j // side != d):
                    r_copy(d, s - 1, j).wait_recv()
                    value = (
                        value.astype(jnp.float32) + landed[d, s - 1, j].astype(jnp.float32)
                    ).astype(jnp.bfloat16)
                sent[d, s, j] = value
                r_copy(d, s, j).start()
    for at in range(CUTS):
        j = at
        value = partial[j, pl.ds(own_slot, block), :].astype(jnp.float32)
        for d in range(2):
            r_copy(d, far - 1, j).wait_recv()
            value = value + landed[d, far - 1, j].astype(jnp.float32)
        cols = pl.ds(j * cut, cut)
        mixed[:, cols] = jnp.sqrt(jnp.float32(2.0)) * tok_in[:, cols].astype(jnp.float32) + 0.5 * value

    loads[5].wait()
    loads[6].wait()

    three = ready.at[pl.ds(0, PARTS), 0, pl.ds(0, share), :]

    def left(sem):
        pltpu.make_async_copy(three, three, sem).wait()

    for j in range(1, nz):

        @pl.when(goes_right & (z >= j - 1))
        def _():
            left(a_send.at[j - 1])

    for j in range(1, left_most + 1):

        @pl.when((goes_left | (z == 1)) & (z + j - 1 <= last_left))
        def _():
            left(b_send.at[j - 1])

    for j in range(TOP):

        @pl.when(passes_top | (z == low + j))
        def _():
            left(c_send.at[j])

    for i in range(PARTS):
        ref = ready.at[all_others, 0, pl.ds(0, share), :]
        pltpu.make_async_copy(ref, ref, core_send.at[i]).wait()
    gone = normed.at[pl.ds(0, 3 * block + half), :]
    for d in range(2):
        pltpu.make_async_copy(gone, gone, x_send.at[d]).wait()
        for ref, at in ((sent.at[d, 0, pl.ds(0, side)], 0), (sent.at[d, pl.ds(1, far - 1)], 1)):
            pltpu.make_async_copy(ref, ref, r_send.at[d, at]).wait()


def finish(units, ready, mixed, affine, gate, up, down, result, put_sem):
    puts = []
    pieces, cols = ready.shape[0], ready.shape[3]
    for m, out in enumerate((gate, up, down)):
        for i in range(pieces):
            puts.append(
                pltpu.make_async_copy(
                    ready.at[i, m, pl.ds(0, units), :], out.at[:, pl.ds(i * cols, cols)], put_sem.at[m, i]
                )
            )
    for put in puts:
        put.start()
    center = jnp.mean(mixed[...], axis=-1, keepdims=True)
    off = mixed[...] - center
    spread = jnp.mean(jnp.square(off), axis=-1, keepdims=True)
    result[...] = (off * lax.rsqrt(spread + 1e-05) * affine[0] + affine[1]).astype(jnp.bfloat16)
    for put in puts:
        put.wait()


def local(n_fs, n_tp, tokens, gate, up, down, norm_gain, post_gain, post_bias):
    block, width = tokens.shape
    piece, units = gate.shape
    nz, far = n_fs // 2, n_tp // 2
    share = -(-units // 32) * 16
    cut = width // CUTS
    bf16, f32 = jnp.bfloat16, jnp.float32
    dma = pltpu.SemaphoreType.DMA
    left_most = max(nz - TOP, TOP) - 1
    ready, mixed, affine = pl.pallas_call(
        functools.partial(gather_and_reduce, n_fs, n_tp, units),
        out_shape=(
            pltpu.VMEM((nz, 3, 2 * share, 2 * piece), bf16),
            pltpu.VMEM((block, width), f32),
            pltpu.VMEM((2, 1, width), f32),
        ),
        in_specs=[HBM_SPACE] * 7,
        out_specs=(VMEM_SPACE, VMEM_SPACE, VMEM_SPACE),
        scratch_shapes=[
            pltpu.VMEM((block, width), bf16),
            pltpu.VMEM((3, 2 * piece, units), f32),
            pltpu.VMEM((1, 2 * piece), f32),
            pltpu.VMEM((n_tp * block, width), bf16),
            pltpu.VMEM((CUTS, n_tp * block, cut), bf16),
            pltpu.VMEM((2, far, CUTS, block, cut), bf16),
            pltpu.VMEM((2, far, CUTS, block, cut), bf16),
            dma((7,)),
            dma((2, 3)),
            dma((nz - 1, PARTS)),
            dma((nz - 1,)),
            dma((left_most, PARTS)),
            dma((left_most,)),
            dma((TOP, PARTS)),
            dma((TOP,)),
            dma((PARTS,)),
            dma((PARTS,)),
            dma((2, far)),
            dma((2,)),
            dma((2, far, CUTS)),
            dma((2, 2)),
            pltpu.SemaphoreType.REGULAR,
        ],
        compiler_params=pltpu.CompilerParams(
            collective_id=0, has_side_effects=True, vmem_limit_bytes=58 * 1024 * 1024
        ),
    )(
        tokens, gate, up, down, norm_gain.reshape(-1, 2 * piece),
        post_gain.reshape(1, -1), post_bias.reshape(1, -1),
    )
    gate_out, up_out, down_out, result = pl.pallas_call(
        functools.partial(finish, units),
        out_shape=(
            pltpu.HBM((units, n_fs * piece), bf16),
            pltpu.HBM((units, n_fs * piece), bf16),
            pltpu.HBM((units, n_fs * piece), bf16),
            jax.ShapeDtypeStruct((block, width), bf16),
        ),
        in_specs=[VMEM_SPACE] * 3,
        out_specs=(HBM_SPACE, HBM_SPACE, HBM_SPACE, VMEM_SPACE),
        scratch_shapes=[dma((3, nz))],
        compiler_params=pltpu.CompilerParams(vmem_limit_bytes=48 * 1024 * 1024),
    )(ready, mixed, affine)
    return gate_out.T, up_out.T, down_out.T, result


def solution(mesh):
    return jax.shard_map(
        functools.partial(local, mesh.shape["fs"], mesh.shape["tp"]),
        mesh=mesh,
        in_specs=(
            P(("grp", "fs", "tp"), None),
            P("fs", "tp"),
            P("fs", "tp"),
            P("fs", "tp"),
            P(),
            P(),
            P(),
        ),
        out_specs=(P("grp", "tp"), P("grp", "tp"), P("grp", "tp"), P(("grp", "fs", "tp"), None)),
        check_vma=False,
    )
```

```python
import functools

import jax
import jax.numpy as jnp
from jax import lax
from jax.experimental import pallas as pl
from jax.experimental.pallas import tpu as pltpu
from jax.sharding import PartitionSpec as P

MESH = pl.DeviceIdType.MESH
CUTS = 8
TOP = 7
HUB = 2
PARTS = 3
VMEM_SPACE = pl.BlockSpec(memory_space=pltpu.VMEM)
HBM_SPACE = pl.BlockSpec(memory_space=pltpu.HBM)


def gather_and_reduce(
    n_fs, n_tp, units, tokens, gate, up, down, gain, post_gain, post_bias, ready, mixed, affine,
    tok_in, w_in, gain_in, normed, partial, sent, landed,
    in_sem, swap_sem, a_recv, a_send, b_recv, b_send, c_recv, c_send, core_recv, core_send,
    x_recv, x_send, r_recv, r_send, first_in, c_left,
):
    f, t = lax.axis_index("fs"), lax.axis_index("tp")
    nz = n_fs // 2
    z, c = f // 2, lax.rem(f, 2)
    low = nz - TOP
    block, width = tok_in.shape
    piece = w_in.shape[1] // 2
    pair_cols = 2 * piece
    share = ready.shape[2] // 2
    far = n_tp // 2
    cut = width // CUTS
    other = f + 1 - 2 * c

    def remote(src, dst, send, recv, **there):
        return pltpu.make_async_remote_copy(
            src_ref=src, dst_ref=dst, send_sem=send, recv_sem=recv,
            device_id=there, device_id_type=MESH,
        )

    def near(step):
        return lax.rem(t + step + n_tp, n_tp)

    barrier = pltpu.get_barrier_semaphore()

    def greet(**there):
        pl.semaphore_signal(barrier, inc=1, device_id=there, device_id_type=MESH)

    greet(fs=other)
    for step in (1, -1, 2, -2):
        greet(tp=near(step))

    @pl.when(z > 0)
    def _():
        greet(fs=f - 2)

    @pl.when((z > 0) & (z < nz - 1))
    def _():
        greet(fs=f + 2)

    @pl.when(z == 0)
    def _():
        for i in range(HUB, TOP):
            greet(fs=c + 2 * (low + i))

    @pl.when(z == 1)
    def _():
        for i in range(HUB):
            greet(fs=c + 2 * (low + i))

    my_rows = pl.ds(pl.multiple_of(c * piece, piece), piece)
    masters = (gate, up, down)
    loads = [pltpu.make_async_copy(tokens, tok_in, in_sem.at[0])]
    loads.append(pltpu.make_async_copy(gain.at[pl.ds(z, 1), :], gain_in, in_sem.at[1]))
    for m in range(3):
        loads.append(pltpu.make_async_copy(masters[m], w_in.at[m, my_rows, :], in_sem.at[2 + m]))
    loads.append(pltpu.make_async_copy(post_gain, affine.at[0], in_sem.at[5]))
    loads.append(pltpu.make_async_copy(post_bias, affine.at[1], in_sem.at[6]))
    for load in loads:
        load.start()

    count = 5 + jnp.where(z > 1, 1, 0) + jnp.where(z < nz - 1, 1, 0) + jnp.where(z >= low, 1, 0)
    pl.semaphore_wait(barrier, count)

    @pl.when(z == 0)
    def _():
        pl.semaphore_signal(first_in, inc=1, device_id={"fs": f + 2}, device_id_type=MESH)

    swaps = []
    for m in range(3):
        swaps.append(remote(masters[m], w_in.at[m, my_rows, :], swap_sem.at[0, m], swap_sem.at[1, m], fs=other))
        swaps[m].start()

    own_slot = (n_tp - 1) * block

    def slot(d, k):
        if k == 0:
            return own_slot
        return (2 * (k - 1) + (d if k < far else 0)) * block

    half = block // 2

    def x_copy(d, k_from, k_to):
        size = half if k_to == far else block
        shift = d * half if k_to == far else 0
        step = k_to - k_from
        return remote(
            normed.at[pl.ds(slot(d, k_from) + shift, size), :],
            normed.at[pl.ds(slot(d, k_to) + shift, size), :],
            x_send.at[d], x_recv.at[d, k_to - 1], tp=near(step if d == 0 else -step),
        )

    loads[1].wait()
    lane = lax.broadcasted_iota(jnp.int32, (pair_cols, pair_cols), 1)
    row = lax.broadcasted_iota(jnp.int32, (pair_cols, pair_cols), 0)
    gain_col = jnp.sum(jnp.where(lane == row, gain_in[...], 0.0), axis=1, keepdims=True)

    for m in range(3):
        loads[2 + m].wait()
        swaps[m].wait()
        value = w_in[m]
        if m < 2:
            value = gain_col * value
        ready[z, m, pl.ds(0, units), :] = value.T.astype(jnp.bfloat16)
        ready[z, m, pl.ds(units, 2 * share - units), :] = jnp.zeros(
            (2 * share - units, pair_cols), jnp.bfloat16
        )

    def part(i, index):
        if i < 2:
            return ready.at[index, c, pl.ds(i * share, share), :]
        return ready.at[index, 2, pl.ds(pl.multiple_of(c * share, 16), share), :]

    def a_copy(i, j, index):
        ref = part(i, index)
        return remote(ref, ref, a_send.at[j - 1], a_recv.at[j - 1, i], fs=f + 2)

    def b_copy(i, j, index):
        ref = part(i, index)
        return remote(ref, ref, b_send.at[j - 1], b_recv.at[j - 1, i], fs=f - 2)

    def c_copy(i, j, index, there):
        ref = part(i, index)
        return remote(ref, ref, c_send.at[j], c_recv.at[j, i], fs=there)

    def c_left_copy(i, j, index):
        ref = part(i, index)
        return remote(ref, ref, c_left.at[j], c_recv.at[j, i], fs=f - 2)

    def core_copy(i, index):
        ref = part(i, index)
        return remote(ref, ref, core_send.at[i], core_recv.at[i], fs=other)

    goes_right = z < nz - 1
    goes_left = (z > 0) & (z != low)
    passes_top = z < low - 1

    @pl.when(z >= low)
    def _():
        for i in range(PARTS):
            c_copy(i, z - low, z, jnp.where(z - low < HUB, 2, 0) + c).start()

    @pl.when(goes_left & (z > 1))
    def _():
        for i in range(PARTS):
            b_copy(i, 1, z).start()

    @pl.when(goes_right)
    def _():
        for i in range(PARTS):
            a_copy(i, 1, z).start()

    loads[0].wait()
    wide = tok_in[...].astype(jnp.float32)
    normed[pl.ds(own_slot, block), :] = (
        wide * lax.rsqrt(jnp.mean(wide * wide, axis=-1, keepdims=True) + 1e-06)
    ).astype(jnp.bfloat16)
    for k in (2, 1):
        for d in range(2):
            x_copy(d, 0, k).start()

    @pl.when(z == 1)
    def _():
        pl.semaphore_wait(first_in, 1)
        for i in range(PARTS):
            b_copy(i, 1, z).start()

    left_most = max(low, TOP) - 1
    last_left = jnp.where(z < low, low - 1, nz - 1)
    events = []
    for j in range(1, nz - 1):
        events.append((5.0 + 3.0 * j, "a", j))
    for j in range(1, left_most + 1):
        events.append((10.0 + 6.0 * j, "b", j))
    for j in range(TOP):
        events.append((2.0 * low + 27.0 + 2.4 * j, "c", j))
    events.append((27.0, "x", 0))
    events.append((2.0 * low + 33.5, "first", 0))
    events.append((1000.0, "end", 0))
    for _, kind, j in sorted(events):
        if kind == "x":
            for d in range(2):
                x_copy(d, 0, 2).wait_recv()
                for k in (far, 3):
                    x_copy(d, 2, k).start()
        if kind == "end":

            @pl.when(z == 0)
            def _():
                for j in range(1, low):
                    for i in range(PARTS):
                        b_copy(i, j, j).wait_recv()
                        core_copy(i, j).start()
                for j in range(HUB):
                    for i in range(PARTS):
                        c_copy(i, j, low + j, c).wait_recv()
                        core_copy(i, low + j).start()

        if kind == "first":

            @pl.when(z > 0)
            def _():
                for i in range(PARTS):
                    a_copy(i, z, 0).wait_recv()

                    @pl.when(goes_right)
                    def _():
                        a_copy(i, z + 1, 0).start()

                    core_copy(i, 0).start()

        if kind == "a":

            @pl.when(z > j)
            def _():
                for i in range(PARTS):
                    a_copy(i, j, z - j).wait_recv()

                    @pl.when(goes_right)
                    def _():
                        a_copy(i, j + 1, z - j).start()

                    core_copy(i, z - j).start()

        if kind == "b":

            @pl.when((z > 0) & (z + j <= last_left))
            def _():
                for i in range(PARTS):
                    b_copy(i, j, z + j).wait_recv()

                    @pl.when(goes_left)
                    def _():
                        b_copy(i, j + 1, z + j).start()

                    core_copy(i, z + j).start()

        if kind == "c":

            @pl.when((z < low) if j >= HUB else (z > 0) & (z < low))
            def _():
                for i in range(PARTS):
                    c_copy(i, j, low + j, c).wait_recv()
                    if j < HUB:

                        @pl.when(z == 1)
                        def _():
                            c_left_copy(i, j, low + j).start()

                    @pl.when(passes_top)
                    def _():
                        c_copy(i, j, low + j, f + 2).start()

                    core_copy(i, low + j).start()

    all_others = pl.ds(0, nz - 1)
    for i in range(PARTS):
        ref = ready.at[all_others, 0, pl.ds(0, share), :]
        pltpu.make_async_copy(ref, ref, core_recv.at[i]).wait()

    def cut_of(m, j):
        each = cut // pair_cols
        return jnp.concatenate([ready[j * each + i, m, pl.ds(0, units), :] for i in range(each)], axis=1)

    def compute(k):
        for d in range(2):
            if k == far:
                x_copy(d, 2, far).wait_recv()
            elif k != 2:
                x_copy(d, 0 if k == 1 else 2, k).wait_recv()
        rows = pl.ds(slot(0, k), 2 * block)
        dims = (((1,), (1,)), ((), ()))
        g = u = None
        for j in range(CUTS):
            x = normed[rows, pl.ds(j * cut, cut)]
            g_more = lax.dot_general(x, cut_of(0, j), dims, preferred_element_type=jnp.float32)
            u_more = lax.dot_general(x, cut_of(1, j), dims, preferred_element_type=jnp.float32)
            g = g_more if j == 0 else g + g_more
            u = u_more if j == 0 else u + u_more
        h = (g * (1.0 / (1.0 + jnp.exp(-g))) * u).astype(jnp.bfloat16)
        for j in range(CUTS):
            partial[j, rows, :] = jnp.dot(
                h, cut_of(2, j), preferred_element_type=jnp.float32
            ).astype(jnp.bfloat16)

    def r_copy(d, s, j):
        return remote(
            sent.at[d, s, j], landed.at[d, s, j], r_send.at[d, min(s, 1)], r_recv.at[d, s, j],
            tp=near(1 - 2 * d),
        )

    side = CUTS // 2
    for s in range(far):
        k = far - s
        compute(k)
        for at in range(side if s == 0 else CUTS):
            for d in range(2):
                j = d * side + at if s == 0 else ((1 - d) * side + at) % CUTS
                value = partial[j, pl.ds(slot(1 - d, k), block), :]
                if s > 0 and not (s == 1 and j // side != d):
                    r_copy(d, s - 1, j).wait_recv()
                    value = (
                        value.astype(jnp.float32) + landed[d, s - 1, j].astype(jnp.float32)
                    ).astype(jnp.bfloat16)
                sent[d, s, j] = value
                r_copy(d, s, j).start()
    for at in range(CUTS):
        j = at
        value = partial[j, pl.ds(own_slot, block), :].astype(jnp.float32)
        for d in range(2):
            r_copy(d, far - 1, j).wait_recv()
            value = value + landed[d, far - 1, j].astype(jnp.float32)
        cols = pl.ds(j * cut, cut)
        mixed[:, cols] = jnp.sqrt(jnp.float32(2.0)) * tok_in[:, cols].astype(jnp.float32) + 0.5 * value

    loads[5].wait()
    loads[6].wait()

    three = ready.at[pl.ds(0, PARTS), 0, pl.ds(0, share), :]

    def left(sem):
        pltpu.make_async_copy(three, three, sem).wait()

    for j in range(1, nz):

        @pl.when(goes_right & (z >= j - 1))
        def _():
            left(a_send.at[j - 1])

    for j in range(1, left_most + 1):

        @pl.when(goes_left & (z + j - 1 <= last_left))
        def _():
            left(b_send.at[j - 1])

    for j in range(TOP):

        passes = passes_top if j >= HUB else passes_top & (z > 0)

        @pl.when(passes | (z == low + j))
        def _():
            left(c_send.at[j])

    @pl.when(z == 1)
    def _():
        for j in range(HUB):
            left(c_left.at[j])

    for i in range(PARTS):
        ref = ready.at[all_others, 0, pl.ds(0, share), :]
        pltpu.make_async_copy(ref, ref, core_send.at[i]).wait()
    gone = normed.at[pl.ds(0, 3 * block + half), :]
    for d in range(2):
        pltpu.make_async_copy(gone, gone, x_send.at[d]).wait()
        for ref, at in ((sent.at[d, 0, pl.ds(0, side)], 0), (sent.at[d, pl.ds(1, far - 1)], 1)):
            pltpu.make_async_copy(ref, ref, r_send.at[d, at]).wait()


def finish(units, ready, mixed, affine, gate, up, down, result, put_sem):
    puts = []
    pieces, cols = ready.shape[0], ready.shape[3]
    for m, out in enumerate((gate, up, down)):
        for i in range(pieces):
            puts.append(
                pltpu.make_async_copy(
                    ready.at[i, m, pl.ds(0, units), :], out.at[:, pl.ds(i * cols, cols)], put_sem.at[m, i]
                )
            )
    for put in puts:
        put.start()
    center = jnp.mean(mixed[...], axis=-1, keepdims=True)
    off = mixed[...] - center
    spread = jnp.mean(jnp.square(off), axis=-1, keepdims=True)
    result[...] = (off * lax.rsqrt(spread + 1e-05) * affine[0] + affine[1]).astype(jnp.bfloat16)
    for put in puts:
        put.wait()


def local(n_fs, n_tp, tokens, gate, up, down, norm_gain, post_gain, post_bias):
    block, width = tokens.shape
    piece, units = gate.shape
    nz, far = n_fs // 2, n_tp // 2
    share = -(-units // 32) * 16
    cut = width // CUTS
    bf16, f32 = jnp.bfloat16, jnp.float32
    dma = pltpu.SemaphoreType.DMA
    left_most = max(nz - TOP, TOP) - 1
    ready, mixed, affine = pl.pallas_call(
        functools.partial(gather_and_reduce, n_fs, n_tp, units),
        out_shape=(
            pltpu.VMEM((nz, 3, 2 * share, 2 * piece), bf16),
            pltpu.VMEM((block, width), f32),
            pltpu.VMEM((2, 1, width), f32),
        ),
        in_specs=[HBM_SPACE] * 7,
        out_specs=(VMEM_SPACE, VMEM_SPACE, VMEM_SPACE),
        scratch_shapes=[
            pltpu.VMEM((block, width), bf16),
            pltpu.VMEM((3, 2 * piece, units), f32),
            pltpu.VMEM((1, 2 * piece), f32),
            pltpu.VMEM((n_tp * block, width), bf16),
            pltpu.VMEM((CUTS, n_tp * block, cut), bf16),
            pltpu.VMEM((2, far, CUTS, block, cut), bf16),
            pltpu.VMEM((2, far, CUTS, block, cut), bf16),
            dma((7,)),
            dma((2, 3)),
            dma((nz - 1, PARTS)),
            dma((nz - 1,)),
            dma((left_most, PARTS)),
            dma((left_most,)),
            dma((TOP, PARTS)),
            dma((TOP,)),
            dma((PARTS,)),
            dma((PARTS,)),
            dma((2, far)),
            dma((2,)),
            dma((2, far, CUTS)),
            dma((2, 2)),
            pltpu.SemaphoreType.REGULAR,
            dma((HUB,)),
        ],
        compiler_params=pltpu.CompilerParams(
            collective_id=0, has_side_effects=True, vmem_limit_bytes=58 * 1024 * 1024
        ),
    )(
        tokens, gate, up, down, norm_gain.reshape(-1, 2 * piece),
        post_gain.reshape(1, -1), post_bias.reshape(1, -1),
    )
    gate_out, up_out, down_out, result = pl.pallas_call(
        functools.partial(finish, units),
        out_shape=(
            pltpu.HBM((units, n_fs * piece), bf16),
            pltpu.HBM((units, n_fs * piece), bf16),
            pltpu.HBM((units, n_fs * piece), bf16),
            jax.ShapeDtypeStruct((block, width), bf16),
        ),
        in_specs=[VMEM_SPACE] * 3,
        out_specs=(HBM_SPACE, HBM_SPACE, HBM_SPACE, VMEM_SPACE),
        scratch_shapes=[dma((3, nz))],
        compiler_params=pltpu.CompilerParams(vmem_limit_bytes=48 * 1024 * 1024),
    )(ready, mixed, affine)
    return gate_out.T, up_out.T, down_out.T, result


def solution(mesh):
    return jax.shard_map(
        functools.partial(local, mesh.shape["fs"], mesh.shape["tp"]),
        mesh=mesh,
        in_specs=(
            P(("grp", "fs", "tp"), None),
            P("fs", "tp"),
            P("fs", "tp"),
            P("fs", "tp"),
            P(),
            P(),
            P(),
        ),
        out_specs=(P("grp", "tp"), P("grp", "tp"), P("grp", "tp"), P(("grp", "fs", "tp"), None)),
        check_vma=False,
    )
```

```python
import functools

import jax
import jax.numpy as jnp
from jax import lax
from jax.experimental import pallas as pl
from jax.experimental.pallas import tpu as pltpu
from jax.sharding import PartitionSpec as P

MESH = pl.DeviceIdType.MESH
CUTS = 8
TOP = 7
HUB = 2
PARTS = 3
VMEM_SPACE = pl.BlockSpec(memory_space=pltpu.VMEM)
HBM_SPACE = pl.BlockSpec(memory_space=pltpu.HBM)


def gather_and_reduce(
    n_fs, n_tp, units, tokens, gate, up, down, gain, post_gain, post_bias, ready, mixed, affine,
    tok_in, w_in, gain_in, normed, partial, sent, landed,
    in_sem, swap_sem, a_recv, a_send, b_recv, b_send, c_recv, c_send, core_recv, core_send,
    x_recv, x_send, r_recv, r_send, first_in, c_left,
):
    f, t = lax.axis_index("fs"), lax.axis_index("tp")
    nz = n_fs // 2
    z, c = f // 2, lax.rem(f, 2)
    low = nz - TOP
    block, width = tok_in.shape
    piece = w_in.shape[1] // 2
    pair_cols = 2 * piece
    share = ready.shape[2] // 2
    far = n_tp // 2
    cut = width // CUTS
    other = f + 1 - 2 * c

    def remote(src, dst, send, recv, **there):
        return pltpu.make_async_remote_copy(
            src_ref=src, dst_ref=dst, send_sem=send, recv_sem=recv,
            device_id=there, device_id_type=MESH,
        )

    def near(step):
        return lax.rem(t + step + n_tp, n_tp)

    barrier = pltpu.get_barrier_semaphore()

    def greet(**there):
        pl.semaphore_signal(barrier, inc=1, device_id=there, device_id_type=MESH)

    greet(fs=other)
    for step in (1, -1, 2, -2):
        greet(tp=near(step))

    @pl.when(z > 0)
    def _():
        greet(fs=f - 2)

    @pl.when((z > 0) & (z < nz - 1))
    def _():
        greet(fs=f + 2)

    @pl.when(z == 0)
    def _():
        for i in range(HUB, TOP):
            greet(fs=c + 2 * (low + i))

    @pl.when(z == 1)
    def _():
        for i in range(HUB):
            greet(fs=c + 2 * (low + i))

    my_rows = pl.ds(pl.multiple_of(c * piece, piece), piece)
    masters = (gate, up, down)
    loads = [pltpu.make_async_copy(tokens, tok_in, in_sem.at[0])]
    loads.append(pltpu.make_async_copy(gain.at[pl.ds(z, 1), :], gain_in, in_sem.at[1]))
    for m in range(3):
        loads.append(pltpu.make_async_copy(masters[m], w_in.at[m, my_rows, :], in_sem.at[2 + m]))
    loads.append(pltpu.make_async_copy(post_gain, affine.at[0], in_sem.at[5]))
    loads.append(pltpu.make_async_copy(post_bias, affine.at[1], in_sem.at[6]))
    for load in loads:
        load.start()

    count = 5 + jnp.where(z > 1, 1, 0) + jnp.where(z < nz - 1, 1, 0) + jnp.where(z >= low, 1, 0)
    pl.semaphore_wait(barrier, count)

    @pl.when(z == 0)
    def _():
        pl.semaphore_signal(first_in, inc=1, device_id={"fs": f + 2}, device_id_type=MESH)

    swaps = []
    for m in range(3):
        swaps.append(remote(masters[m], w_in.at[m, my_rows, :], swap_sem.at[0, m], swap_sem.at[1, m], fs=other))
        swaps[m].start()

    own_slot = (n_tp - 1) * block

    def slot(d, k):
        if k == 0:
            return own_slot
        return (2 * (k - 1) + (d if k < far else 0)) * block

    half = block // 2

    def x_copy(d, k_from, k_to):
        size = half if k_to == far else block
        shift = d * half if k_to == far else 0
        step = k_to - k_from
        return remote(
            normed.at[pl.ds(slot(d, k_from) + shift, size), :],
            normed.at[pl.ds(slot(d, k_to) + shift, size), :],
            x_send.at[d], x_recv.at[d, k_to - 1], tp=near(step if d == 0 else -step),
        )

    loads[1].wait()
    lane = lax.broadcasted_iota(jnp.int32, (pair_cols, pair_cols), 1)
    row = lax.broadcasted_iota(jnp.int32, (pair_cols, pair_cols), 0)
    gain_col = jnp.sum(jnp.where(lane == row, gain_in[...], 0.0), axis=1, keepdims=True)

    for m in range(3):
        loads[2 + m].wait()
        swaps[m].wait()
        value = w_in[m]
        if m < 2:
            value = gain_col * value
        ready[z, m, pl.ds(0, units), :] = value.T.astype(jnp.bfloat16)
        ready[z, m, pl.ds(units, 2 * share - units), :] = jnp.zeros(
            (2 * share - units, pair_cols), jnp.bfloat16
        )

    def part(i, index):
        if i < 2:
            return ready.at[index, c, pl.ds(i * share, share), :]
        return ready.at[index, 2, pl.ds(pl.multiple_of(c * share, 16), share), :]

    def a_copy(i, j, index):
        ref = part(i, index)
        return remote(ref, ref, a_send.at[j - 1], a_recv.at[j - 1, i], fs=f + 2)

    def b_copy(i, j, index):
        ref = part(i, index)
        return remote(ref, ref, b_send.at[j - 1], b_recv.at[j - 1, i], fs=f - 2)

    def c_copy(i, j, index, there):
        ref = part(i, index)
        return remote(ref, ref, c_send.at[j], c_recv.at[j, i], fs=there)

    def c_left_copy(i, j, index):
        ref = part(i, index)
        return remote(ref, ref, c_left.at[j], c_recv.at[j, i], fs=f - 2)

    def core_copy(i, index):
        ref = part(i, index)
        return remote(ref, ref, core_send.at[i], core_recv.at[i], fs=other)

    goes_right = z < nz - 1
    goes_left = (z > 0) & (z != low)
    passes_top = z < low - 1

    @pl.when(z >= low)
    def _():
        for i in range(PARTS):
            c_copy(i, z - low, z, jnp.where(z - low < HUB, 2, 0) + c).start()

    @pl.when(goes_left & (z > 1))
    def _():
        for i in range(PARTS):
            b_copy(i, 1, z).start()

    @pl.when(goes_right)
    def _():
        for i in range(PARTS):
            a_copy(i, 1, z).start()

    loads[0].wait()
    wide = tok_in[...].astype(jnp.float32)
    normed[pl.ds(own_slot, block), :] = (
        wide * lax.rsqrt(jnp.mean(wide * wide, axis=-1, keepdims=True) + 1e-06)
    ).astype(jnp.bfloat16)
    for k in (2, 1):
        for d in range(2):
            x_copy(d, 0, k).start()

    @pl.when(z == 1)
    def _():
        pl.semaphore_wait(first_in, 1)
        for i in range(PARTS):
            b_copy(i, 1, z).start()

    left_most = max(low, TOP) - 1
    last_left = jnp.where(z < low, low - 1, nz - 1)
    events = []
    for j in range(1, nz - 1):
        events.append((5.0 + 3.0 * j, "a", j))
    for j in range(1, left_most + 1):
        events.append((10.0 + 6.0 * j, "b", j))
    for j in range(TOP):
        events.append((2.0 * low + 27.0 + 2.4 * j, "c", j))
    events.append((27.0, "x", 0))
    events.append((2.0 * low + 33.5, "first", 0))
    events.append((1000.0, "end", 0))
    for _, kind, j in sorted(events):
        if kind == "x":
            for d in range(2):
                x_copy(d, 0, 2).wait_recv()
                for k in (far, 3):
                    x_copy(d, 2, k).start()
        if kind == "end":

            @pl.when(z == 0)
            def _():
                for j in range(1, low):
                    for i in range(PARTS):
                        b_copy(i, j, j).wait_recv()
                        core_copy(i, j).start()
                for j in range(HUB):
                    for i in range(PARTS):
                        c_copy(i, j, low + j, c).wait_recv()
                        core_copy(i, low + j).start()

        if kind == "first":

            @pl.when(z > 0)
            def _():
                for i in range(PARTS):
                    a_copy(i, z, 0).wait_recv()

                    @pl.when(goes_right)
                    def _():
                        a_copy(i, z + 1, 0).start()

                    core_copy(i, 0).start()

        if kind == "a":

            @pl.when(z > j)
            def _():
                for i in range(PARTS):
                    a_copy(i, j, z - j).wait_recv()

                    @pl.when(goes_right)
                    def _():
                        a_copy(i, j + 1, z - j).start()

                    core_copy(i, z - j).start()

        if kind == "b":

            @pl.when((z > 0) & (z + j <= last_left))
            def _():
                for i in range(PARTS):
                    b_copy(i, j, z + j).wait_recv()

                    @pl.when(goes_left)
                    def _():
                        b_copy(i, j + 1, z + j).start()

                    core_copy(i, z + j).start()

        if kind == "c":

            @pl.when((z < low) if j >= HUB else (z > 0) & (z < low))
            def _():
                for i in range(PARTS):
                    c_copy(i, j, low + j, c).wait_recv()
                    if j < HUB:

                        @pl.when(z == 1)
                        def _():
                            c_left_copy(i, j, low + j).start()

                    @pl.when(passes_top)
                    def _():
                        c_copy(i, j, low + j, f + 2).start()

                    core_copy(i, low + j).start()

    all_others = pl.ds(0, nz - 1)
    for i in range(PARTS):
        ref = ready.at[all_others, 0, pl.ds(0, share), :]
        pltpu.make_async_copy(ref, ref, core_recv.at[i]).wait()

    def cut_of(m, j):
        each = cut // pair_cols
        return jnp.concatenate([ready[j * each + i, m, pl.ds(0, units), :] for i in range(each)], axis=1)

    def compute(k):
        for d in range(2):
            if k == far:
                x_copy(d, 2, far).wait_recv()
            elif k != 2:
                x_copy(d, 0 if k == 1 else 2, k).wait_recv()
        rows = pl.ds(slot(0, k), 2 * block)
        dims = (((1,), (1,)), ((), ()))
        g = u = None
        for j in range(CUTS):
            x = normed[rows, pl.ds(j * cut, cut)]
            g_more = lax.dot_general(x, cut_of(0, j), dims, preferred_element_type=jnp.float32)
            u_more = lax.dot_general(x, cut_of(1, j), dims, preferred_element_type=jnp.float32)
            g = g_more if j == 0 else g + g_more
            u = u_more if j == 0 else u + u_more
        h = (g * (1.0 / (1.0 + jnp.exp(-g))) * u).astype(jnp.bfloat16)
        done = set()

        def ensure(j):
            if j not in done:
                done.add(j)
                partial[j, rows, :] = jnp.dot(
                    h, cut_of(2, j), preferred_element_type=jnp.float32
                ).astype(jnp.bfloat16)

        return ensure

    def r_copy(d, s, j):
        return remote(
            sent.at[d, s, j], landed.at[d, s, j], r_send.at[d, min(s, 1)], r_recv.at[d, s, j],
            tp=near(1 - 2 * d),
        )

    side = CUTS // 2
    for s in range(far):
        k = far - s
        ensure = compute(k)
        for at in range(side if s == 0 else CUTS):
            for d in range(2):
                j = d * side + at if s == 0 else ((1 - d) * side + at) % CUTS
                ensure(j)
                value = partial[j, pl.ds(slot(1 - d, k), block), :]
                if s > 0 and not (s == 1 and j // side != d):
                    r_copy(d, s - 1, j).wait_recv()
                    value = (
                        value.astype(jnp.float32) + landed[d, s - 1, j].astype(jnp.float32)
                    ).astype(jnp.bfloat16)
                sent[d, s, j] = value
                r_copy(d, s, j).start()
    for at in range(CUTS):
        j = at
        value = partial[j, pl.ds(own_slot, block), :].astype(jnp.float32)
        for d in range(2):
            r_copy(d, far - 1, j).wait_recv()
            value = value + landed[d, far - 1, j].astype(jnp.float32)
        cols = pl.ds(j * cut, cut)
        mixed[:, cols] = jnp.sqrt(jnp.float32(2.0)) * tok_in[:, cols].astype(jnp.float32) + 0.5 * value

    loads[5].wait()
    loads[6].wait()

    three = ready.at[pl.ds(0, PARTS), 0, pl.ds(0, share), :]

    def left(sem):
        pltpu.make_async_copy(three, three, sem).wait()

    for j in range(1, nz):

        @pl.when(goes_right & (z >= j - 1))
        def _():
            left(a_send.at[j - 1])

    for j in range(1, left_most + 1):

        @pl.when(goes_left & (z + j - 1 <= last_left))
        def _():
            left(b_send.at[j - 1])

    for j in range(TOP):

        passes = passes_top if j >= HUB else passes_top & (z > 0)

        @pl.when(passes | (z == low + j))
        def _():
            left(c_send.at[j])

    @pl.when(z == 1)
    def _():
        for j in range(HUB):
            left(c_left.at[j])

    for i in range(PARTS):
        ref = ready.at[all_others, 0, pl.ds(0, share), :]
        pltpu.make_async_copy(ref, ref, core_send.at[i]).wait()
    gone = normed.at[pl.ds(0, 3 * block + half), :]
    for d in range(2):
        pltpu.make_async_copy(gone, gone, x_send.at[d]).wait()
        for ref, at in ((sent.at[d, 0, pl.ds(0, side)], 0), (sent.at[d, pl.ds(1, far - 1)], 1)):
            pltpu.make_async_copy(ref, ref, r_send.at[d, at]).wait()


def finish(units, ready, mixed, affine, gate, up, down, result, put_sem):
    puts = []
    pieces, cols = ready.shape[0], ready.shape[3]
    for m, out in enumerate((gate, up, down)):
        for i in range(pieces):
            puts.append(
                pltpu.make_async_copy(
                    ready.at[i, m, pl.ds(0, units), :], out.at[:, pl.ds(i * cols, cols)], put_sem.at[m, i]
                )
            )
    for put in puts:
        put.start()
    center = jnp.mean(mixed[...], axis=-1, keepdims=True)
    off = mixed[...] - center
    spread = jnp.mean(jnp.square(off), axis=-1, keepdims=True)
    result[...] = (off * lax.rsqrt(spread + 1e-05) * affine[0] + affine[1]).astype(jnp.bfloat16)
    for put in puts:
        put.wait()


def local(n_fs, n_tp, tokens, gate, up, down, norm_gain, post_gain, post_bias):
    block, width = tokens.shape
    piece, units = gate.shape
    nz, far = n_fs // 2, n_tp // 2
    share = -(-units // 32) * 16
    cut = width // CUTS
    bf16, f32 = jnp.bfloat16, jnp.float32
    dma = pltpu.SemaphoreType.DMA
    left_most = max(nz - TOP, TOP) - 1
    ready, mixed, affine = pl.pallas_call(
        functools.partial(gather_and_reduce, n_fs, n_tp, units),
        out_shape=(
            pltpu.VMEM((nz, 3, 2 * share, 2 * piece), bf16),
            pltpu.VMEM((block, width), f32),
            pltpu.VMEM((2, 1, width), f32),
        ),
        in_specs=[HBM_SPACE] * 7,
        out_specs=(VMEM_SPACE, VMEM_SPACE, VMEM_SPACE),
        scratch_shapes=[
            pltpu.VMEM((block, width), bf16),
            pltpu.VMEM((3, 2 * piece, units), f32),
            pltpu.VMEM((1, 2 * piece), f32),
            pltpu.VMEM((n_tp * block, width), bf16),
            pltpu.VMEM((CUTS, n_tp * block, cut), bf16),
            pltpu.VMEM((2, far, CUTS, block, cut), bf16),
            pltpu.VMEM((2, far, CUTS, block, cut), bf16),
            dma((7,)),
            dma((2, 3)),
            dma((nz - 1, PARTS)),
            dma((nz - 1,)),
            dma((left_most, PARTS)),
            dma((left_most,)),
            dma((TOP, PARTS)),
            dma((TOP,)),
            dma((PARTS,)),
            dma((PARTS,)),
            dma((2, far)),
            dma((2,)),
            dma((2, far, CUTS)),
            dma((2, 2)),
            pltpu.SemaphoreType.REGULAR,
            dma((HUB,)),
        ],
        compiler_params=pltpu.CompilerParams(
            collective_id=0, has_side_effects=True, vmem_limit_bytes=58 * 1024 * 1024
        ),
    )(
        tokens, gate, up, down, norm_gain.reshape(-1, 2 * piece),
        post_gain.reshape(1, -1), post_bias.reshape(1, -1),
    )
    gate_out, up_out, down_out, result = pl.pallas_call(
        functools.partial(finish, units),
        out_shape=(
            pltpu.HBM((units, n_fs * piece), bf16),
            pltpu.HBM((units, n_fs * piece), bf16),
            pltpu.HBM((units, n_fs * piece), bf16),
            jax.ShapeDtypeStruct((block, width), bf16),
        ),
        in_specs=[VMEM_SPACE] * 3,
        out_specs=(HBM_SPACE, HBM_SPACE, HBM_SPACE, VMEM_SPACE),
        scratch_shapes=[dma((3, nz))],
        compiler_params=pltpu.CompilerParams(vmem_limit_bytes=48 * 1024 * 1024),
    )(ready, mixed, affine)
    return gate_out.T, up_out.T, down_out.T, result


def solution(mesh):
    return jax.shard_map(
        functools.partial(local, mesh.shape["fs"], mesh.shape["tp"]),
        mesh=mesh,
        in_specs=(
            P(("grp", "fs", "tp"), None),
            P("fs", "tp"),
            P("fs", "tp"),
            P("fs", "tp"),
            P(),
            P(),
            P(),
        ),
        out_specs=(P("grp", "tp"), P("grp", "tp"), P("grp", "tp"), P(("grp", "fs", "tp"), None)),
        check_vma=False,
    )
```
